32 devices in a mesh: fs: 8 (over z, x), tp: 4 (over y, core).
Axes of the slice: x: 2, y: 2, z: 4, core: 2. Of those that a mesh axis runs over, the one named last changes fastest.
Arguments:
- normed_input: bfloat16 [16384, 2048], P('fs'), may hold values from -6 to 6
- forget_cot: bfloat16 [16384, 2048], P('fs', 'tp'), may hold values from -6 to 6
- value_cot: bfloat16 [16384, 2048], P('fs', 'tp'), may hold values from -6 to 6
- gated_output: bfloat16 [16384, 2048], P('fs', 'tp'), may hold values from -6 to 6
- output_cot: bfloat16 [16384, 2048], P('fs'), may hold values from -6 to 6
- forget_weight: float32 [2048, 2048], P('fs', 'tp'), may hold values from -0.125 to 0.125
- value_weight: float32 [2048, 2048], P('fs', 'tp'), may hold values from -0.125 to 0.125
- out_weight: float32 [2048, 2048], P('tp', 'fs'), may hold values from -0.125 to 0.125
- bases: bfloat16 [3, 2048, 256], replicated, may hold values from -0.125 to 0.125
- first_moment: float32 [256, 3, 2048], P('fs', None, 'tp'), may hold values from -4 to 4
- second_moment: float32 [256, 3, 2048], P('fs', None, 'tp'), may hold values from 0.25 to 4
Outputs:
- new_forget: float32 [2048, 2048], P('fs', 'tp')
- new_value: float32 [2048, 2048], P('fs', 'tp')
- new_out: float32 [2048, 2048], P('tp', 'fs')
- copy_forget: bfloat16 [2048, 2048], P(None, 'tp')
- copy_value: bfloat16 [2048, 2048], P(None, 'tp')
- copy_out: bfloat16 [2048, 2048], P('tp')
- moment_one: float32 [256, 3, 2048], P('fs', None, 'tp')
- moment_two: float32 [256, 3, 2048], P('fs', None, 'tp')
- step_forget: float32 [2048, 2048], P('fs', 'tp')
- step_value: float32 [2048, 2048], P('fs', 'tp')
- step_out: float32 [2048, 2048], P('tp', 'fs')
The draws below stay inside these ranges and needn't reach their ends.
All inputs are finite; a program needn't handle non-finite values.
Results may differ from the reference program's by a relative error of at most 0.0045.
Values may be sent and summed in bfloat16 or wider, within the bound.
A program may use at most 128 MiB of HBM per device.

```python
import math
import jax
import jax.numpy as jnp
from jax import lax

D = 2048
QK = 2048
V = 2048
RANK = 256
TOKENS = 16384


def draw_first_moment(key, part):
    base = jax.random.normal(key, (RANK, 3, QK), jnp.float32) * 0.5
    return jnp.clip(base, -4.0, 4.0)


def level_of(rng, dims, shards, smallest, top_value):
    gain = 1.0
    for dim, shards_of in shards:
        heights = jax.random.uniform(jax.random.fold_in(jax.random.fold_in(rng, 6), dim), (shards_of,), jnp.float32, smallest / len(shards), top_value / len(shards))
        gain = gain * jnp.repeat(jnp.exp(heights), dims[dim] // shards_of).reshape((-1,) + (1,) * (len(dims) - 1 - dim))
    return gain


def normal_values(rng, extent, spread, reach, shards=(), dtype=jnp.bfloat16):
    values = spread * jax.random.normal(rng, extent, jnp.float32)
    if shards:
        values = values * level_of(rng, extent, shards, -0.22, 0.18)
    return jnp.clip(values, -reach, reach).astype(dtype)


def setup_inputs(seed: int = 0) -> dict:
    arg_keys = jax.random.split(jax.random.key(seed), 12)
    normed_input = normal_values(arg_keys[0], (TOKENS, D), 1.0, 6.0, ((0, 8),))
    forget_cot = normal_values(arg_keys[1], (TOKENS, QK), 1.0, 6.0, ((0, 8), (1, 4)))
    value_cot = normal_values(arg_keys[2], (TOKENS, V), 1.0, 6.0, ((0, 8), (1, 4)))
    gated_output = normal_values(arg_keys[3], (TOKENS, V), 1.0, 6.0, ((0, 8), (1, 4)))
    output_cot = normal_values(arg_keys[4], (TOKENS, D), 1.0, 6.0, ((0, 8),))
    forget_weight = normal_values(arg_keys[5], (D, QK), D ** -0.5, 0.125, ((0, 8), (1, 4)), jnp.float32)
    value_weight = normal_values(arg_keys[6], (D, V), D ** -0.5, 0.125, ((0, 8), (1, 4)), jnp.float32)
    out_weight = normal_values(arg_keys[7], (V, D), V ** -0.5, 0.125, ((0, 4), (1, 8)), jnp.float32)
    bases = normal_values(arg_keys[8], (3, D, RANK), D ** -0.5, 0.125)
    first_moment = draw_first_moment(jax.random.fold_in(arg_keys[11], 71), 0)
    second_moment = jnp.clip(jnp.exp(math.log(4.0) - 2.7725887 * jax.random.uniform(arg_keys[10], (RANK, 3, QK), jnp.float32) ** level_of(arg_keys[10], (RANK, 3, QK), ((0, 8), (2, 4)), -0.2, 0.2)), 0.25, 4.0)
    return {"normed_input": normed_input, "forget_cot": forget_cot, "value_cot": value_cot, "gated_output": gated_output, "output_cot": output_cot, "forget_weight": forget_weight, "value_weight": value_weight, "out_weight": out_weight, "bases": bases, "first_moment": first_moment, "second_moment": second_moment}


def reference(normed_input, forget_cot, value_cot, gated_output, output_cot, forget_weight, value_weight, out_weight, bases, first_moment, second_moment):
    factor = float(TOKENS) ** (-0.5)
    grad_forget = jnp.dot(normed_input.T, forget_cot, preferred_element_type=jnp.float32) * factor
    grad_value = jnp.dot(normed_input.T, value_cot, preferred_element_type=jnp.float32) * factor
    grad_out = jnp.dot(output_cot.T, gated_output, preferred_element_type=jnp.float32) * factor
    grads = jnp.stack([grad_forget, grad_value, grad_out], axis=1)
    basis_full = bases.astype(jnp.float32)
    projected = jnp.einsum('kdr,dkc->rkc', basis_full, grads, precision=lax.Precision.HIGHEST)
    moment_one = 0.9 * first_moment + 0.1 * projected
    moment_two = 0.9 * second_moment + 0.1 * projected * projected
    direction = moment_one / (jnp.sqrt(moment_two) + 1e-08)
    scale = lax.rsqrt(lax.optimization_barrier(jnp.mean(direction * direction, axis=(0, 2))) + 1.0)
    full = jnp.einsum('kdr,rkc->dkc', basis_full, direction, precision=lax.Precision.HIGHEST)
    full = full * scale[None, :, None]
    step_forget = full[:, 0, :]
    step_value = full[:, 1, :]
    step_out = full[:, 2, :].T
    new_forget = forget_weight - 0.01 * step_forget
    new_value = value_weight - 0.01 * step_value
    new_out = out_weight - 0.01 * step_out
    return (new_forget, new_value, new_out, new_forget.astype(jnp.bfloat16), new_value.astype(jnp.bfloat16), new_out.astype(jnp.bfloat16), moment_one, moment_two, step_forget, step_value, step_out)
```

```python
import functools

import jax
import jax.numpy as jnp
from jax import lax
from jax.experimental import pallas as pl
from jax.experimental.pallas import tpu as pltpu
from jax.sharding import PartitionSpec as P

MESH = pl.DeviceIdType.MESH


def ring_index(place, size):
    back = lax.div(place, size // 2)
    return (1 - back) * 2 * place + back * (2 * (size - 1 - place) + 1)


def ring_place(index, size):
    odd = lax.rem(index, 2)
    half = lax.div(index, 2)
    return (1 - odd) * half + odd * (size - 1 - half)


def exchange_kernel(
    size,
    groups,
    factor,
    entries,
    x_hbm,
    oc_hbm,
    fc_hbm,
    vc_hbm,
    go_hbm,
    bases_hbm,
    fw_ref,
    vw_ref,
    ow_ref,
    m1_ref,
    m2_ref,
    all_f,
    all_v,
    all_o,
    dirs_out,
    scale_ref,
    n1_ref,
    n2_ref,
    x_buf,
    oc_buf,
    c_buf,
    b_buf,
    wf_buf,
    wv_buf,
    wo_buf,
    acc,
    part,
    got,
    mine,
    dirs,
    sums,
    load_sem,
    base_sem,
    put_sem,
    ring_send,
    ring_recv,
    part_send,
    part_recv,
    dir_send,
    dir_recv,
    sum_send,
    sum_recv,
):
    me = lax.axis_index("fs")
    mt = lax.axis_index("tp")
    place = ring_place(me, size)
    right = ring_index(lax.rem(place + 1, size), size)
    left = ring_index(lax.rem(place + size - 1, size), size)
    steps = size // 2
    tiles = load_sem.shape[1]
    tokens = x_buf.shape[0]
    rows_t = tokens // tiles
    rank_rows = m1_ref.shape[1]
    columns = m1_ref.shape[2]

    loads = []
    base_copies = [
        pltpu.make_async_copy(bases_hbm.at[k], b_buf.at[k], base_sem.at[k]) for k in range(3)
    ]

    def load(which, src, dst, tile):
        at = pl.ds(pl.multiple_of(tile * rows_t, rows_t), rows_t)
        return pltpu.make_async_copy(src.at[at, :], dst.at[at, :], load_sem.at[which, tile])

    streams = (
        (x_hbm, x_buf),
        (fc_hbm, c_buf.at[0]),
        (vc_hbm, c_buf.at[1]),
        (oc_hbm, oc_buf),
        (go_hbm, c_buf.at[2]),
    )
    base_copies[0].start()
    for tile in range(tiles):
        for which in (0, 1):
            load(which, *streams[which], tile).start()
    base_copies[1].start()
    for tile in range(tiles):
        load(2, *streams[2], tile).start()
    base_copies[2].start()
    for tile in range(tiles):
        for which in (3, 4):
            load(which, *streams[which], tile).start()

    barrier = pltpu.get_barrier_semaphore()
    for j in range(1, size):
        pl.semaphore_signal(
            barrier, inc=1, device_id=(lax.rem(me + j, size), mt), device_id_type=MESH
        )
    for j in range(1, groups):
        pl.semaphore_signal(
            barrier, inc=1, device_id=(me, lax.rem(mt + j, groups)), device_id_type=MESH
        )
    wf_buf[...] = fw_ref[...].astype(jnp.bfloat16)
    wv_buf[...] = vw_ref[...].astype(jnp.bfloat16)
    wo_buf[...] = ow_ref[...].astype(jnp.bfloat16)
    pl.semaphore_wait(barrier, size - 1 + groups - 1)

    def row_block(ref, owner, half):
        rows = wf_buf.shape[0]
        start, count = owner * rows, rows
        if half is not None:
            count = rows // 2
            start = start + half * count
        return ref.at[pl.ds(pl.multiple_of(start, count), count), :]

    def column_block(ref, owner, half):
        width = wo_buf.shape[1]
        lanes = pl.ds(pl.multiple_of(owner * width, width), width)
        height = wo_buf.shape[0]
        if half is None:
            return ref.at[:, lanes]
        return ref.at[pl.ds(half * (height // 2), height // 2), lanes]

    def dir_block(k, owner, half):
        at = pl.ds(pl.multiple_of(owner * rank_rows, rank_rows), rank_rows)
        if half is None:
            return dirs.at[k, at, :]
        return dirs.at[k, at, pl.ds(half * (columns // 2), columns // 2)]

    items = (
        (wf_buf, functools.partial(row_block, all_f)),
        (wv_buf, functools.partial(row_block, all_v)),
        (wo_buf, functools.partial(column_block, all_o)),
    )

    def hop(view, own, send_sem, recv_sem, item, step, way):
        sign = 1 if way == 0 else size - 1
        owner = ring_index(lax.rem(place + (size - sign) * (step - 1), size), size)
        half = way if step == steps else None
        dst = view(owner, half)
        src = own if own is not None and step == 1 and half is None else dst
        return pltpu.make_async_remote_copy(
            src_ref=src,
            dst_ref=dst,
            send_sem=send_sem.at[way, item, step - 1],
            recv_sem=recv_sem.at[way, item, step - 1],
            device_id=(right if way == 0 else left, mt),
            device_id_type=MESH,
        )

    def weight_hop(item, step, way):
        own, view = items[item]
        return hop(view, own, ring_send, ring_recv, item, step, way)

    def dir_hop(k, step, way):
        own = mine.at[k]
        return hop(functools.partial(dir_block, k), own, dir_send, dir_recv, k, step, way)

    puts = []
    for item in range(3):
        own, view = items[item]
        put = pltpu.make_async_copy(own, view(me, None), put_sem.at[item])
        put.start()
        puts.append(put)
        for way in range(2):
            weight_hop(item, 1, way).start()

    forwards = [(step, item) for step in range(2, steps + 1) for item in range(3)]

    def pump(count):
        for _ in range(min(count, len(forwards))):
            step, item = forwards.pop(0)
            for way in range(2):
                weight_hop(item, step - 1, way).wait_recv()
                weight_hop(item, step, way).start()

    def part_copy(k, j):
        owner = lax.rem(me + j, size)
        at = pl.ds(pl.multiple_of(owner * rank_rows, rank_rows), rank_rows)
        return pltpu.make_async_remote_copy(
            src_ref=part.at[k, at, :],
            dst_ref=got.at[k, j - 1],
            send_sem=part_send.at[k, j - 1],
            recv_sem=part_recv.at[k, j - 1],
            device_id=(owner, mt),
            device_id_type=MESH,
        )

    for k in range(3):
        base_copies[k].wait()
        left_which, right_which = ((0, 1), (0, 2), (3, 4))[k]
        source = x_buf if k < 2 else oc_buf
        acc[k] = jnp.zeros(acc.shape[1:], acc.dtype)

        def tile_body(tile, carry, k=k, left_which=left_which, right_which=right_which, source=source):
            at = pl.ds(pl.multiple_of(tile * rows_t, rows_t), rows_t)
            if k != 1:
                load(left_which, *streams[left_which], tile).wait()
            reduced = jnp.dot(
                source[at, :], b_buf[k], preferred_element_type=jnp.float32
            ).astype(jnp.bfloat16)
            load(right_which, *streams[right_which], tile).wait()
            acc[k] += lax.dot_general(
                reduced,
                c_buf[k, at, :],
                (((0,), (0,)), ((), ())),
                preferred_element_type=jnp.float32,
            )
            return carry

        lax.fori_loop(0, tiles, tile_body, 0)
        part[k] = (acc[k] * factor).astype(jnp.bfloat16)
        for j in range(1, size):
            part_copy(k, j).start()
        pump(1)

    own_rows = pl.ds(pl.multiple_of(me * rank_rows, rank_rows), rank_rows)
    for k in range(3):
        projected = acc[k, own_rows, :] * factor
        for j in range(1, size):
            part_copy(k, j).wait_recv()
            projected = projected + got[k, j - 1].astype(jnp.float32)
        one = 0.9 * m1_ref[k] + 0.1 * projected
        two = 0.9 * m2_ref[k] + 0.1 * projected * projected
        n1_ref[k] = one
        n2_ref[k] = two
        rounded = (one / (jnp.sqrt(two) + 1e-08)).astype(jnp.bfloat16)
        mine[k] = rounded
        dirs[k, own_rows, :] = rounded
        for way in range(2):
            dir_hop(k, 1, way).start()
    pump(3)
    for step in range(2, steps + 1):
        for k in range(3):
            for way in range(2):
                dir_hop(k, step - 1, way).wait_recv()
                dir_hop(k, step, way).start()
        if step == 3:
            pump(3)
    pump(len(forwards))
    for k in range(3):
        for way in range(2):
            dir_hop(k, steps, way).wait_recv()

    dirs_put = pltpu.make_async_copy(dirs, dirs_out, put_sem.at[3])
    dirs_put.start()

    row = lax.broadcasted_iota(jnp.int32, scale_ref.shape, 0)
    tile_sum = jnp.zeros(scale_ref.shape, jnp.float32)
    for k in range(3):
        values = dirs[k].astype(jnp.float32)
        tile_sum = tile_sum + jnp.where(row == k, jnp.sum(values * values), 0.0)
    sums[0] = tile_sum

    def sum_copy(j):
        return pltpu.make_async_remote_copy(
            src_ref=sums.at[0],
            dst_ref=sums.at[j],
            send_sem=sum_send.at[j],
            recv_sem=sum_recv.at[j],
            device_id=(me, lax.rem(mt + j, groups)),
            device_id_type=MESH,
        )

    for j in range(1, groups):
        sum_copy(j).start()
    total = tile_sum
    for j in range(1, groups):
        sum_copy(j).wait_recv()
        total = total + sums[j]
    scale_ref[...] = lax.rsqrt(total / entries + 1.0)

    for item in range(3):
        for way in range(2):
            weight_hop(item, steps, way).wait_recv()
    for put in puts:
        put.wait()
    dirs_put.wait()
    for k in range(3):
        for step in range(1, steps + 1):
            for way in range(2):
                weight_hop(k, step, way).wait_send()
                dir_hop(k, step, way).wait_send()
        for j in range(1, size):
            part_copy(k, j).wait_send()
    for j in range(1, groups):
        sum_copy(j).wait_send()


def exchange(size, groups, x, oc, fc, vc, go, bases, fw, vw, ow, m1, m2):
    tokens, width = x.shape
    rank = bases.shape[2]
    rows, columns = fw.shape
    rank_rows = m1.shape[1]
    steps = size // 2
    tiles = 4
    bf16, f32 = jnp.bfloat16, jnp.float32
    hbm = pl.BlockSpec(memory_space=pl.ANY)
    vmem = pl.BlockSpec(memory_space=pltpu.VMEM)
    dma = pltpu.SemaphoreType.DMA
    kernel = functools.partial(
        exchange_kernel,
        size,
        groups,
        float(tokens * size) ** (-0.5),
        float(rank * columns * groups),
    )
    return pl.pallas_call(
        kernel,
        out_shape=(
            jax.ShapeDtypeStruct((rows * size, columns), bf16),
            jax.ShapeDtypeStruct((rows * size, columns), bf16),
            jax.ShapeDtypeStruct((ow.shape[0], ow.shape[1] * size), bf16),
            jax.ShapeDtypeStruct((3, rank, columns), bf16),
            jax.ShapeDtypeStruct((8, 128), f32),
            jax.ShapeDtypeStruct(m1.shape, f32),
            jax.ShapeDtypeStruct(m2.shape, f32),
        ),
        in_specs=[hbm] * 6 + [vmem] * 5,
        out_specs=(hbm,) * 4 + (vmem,) * 3,
        scratch_shapes=[
            pltpu.VMEM(x.shape, bf16),
            pltpu.VMEM(oc.shape, bf16),
            pltpu.VMEM((3, tokens, columns), bf16),
            pltpu.VMEM(bases.shape, bf16),
            pltpu.VMEM(fw.shape, bf16),
            pltpu.VMEM(vw.shape, bf16),
            pltpu.VMEM(ow.shape, bf16),
            pltpu.VMEM((3, rank, columns), f32),
            pltpu.VMEM((3, rank, columns), bf16),
            pltpu.VMEM((3, size - 1, rank_rows, columns), bf16),
            pltpu.VMEM((3, rank_rows, columns), bf16),
            pltpu.VMEM((3, rank, columns), bf16),
            pltpu.VMEM((groups, 8, 128), f32),
            dma((5, tiles)),
            dma((3,)),
            dma((4,)),
            dma((2, 3, steps)),
            dma((2, 3, steps)),
            dma((3, size - 1)),
            dma((3, size - 1)),
            dma((2, 3, steps)),
            dma((2, 3, steps)),
            dma((groups,)),
            dma((groups,)),
        ],
        compiler_params=pltpu.CompilerParams(
            collective_id=0, has_side_effects=True, vmem_limit_bytes=46 * 1024 * 1024
        ),
    )(x, oc, fc, vc, go, bases, fw, vw, ow, m1, m2)


def on_device(
    normed_input,
    forget_cot,
    value_cot,
    gated_output,
    output_cot,
    forget_weight,
    value_weight,
    out_weight,
    bases,
    first_moment,
    second_moment,
):
    size, groups = lax.axis_size("fs"), lax.axis_size("tp")
    rows = forget_weight.shape[0]
    old_f, old_v, old_o, dirs, scales, one, two = exchange(
        size,
        groups,
        normed_input,
        output_cot,
        forget_cot,
        value_cot,
        gated_output,
        bases,
        forget_weight,
        value_weight,
        out_weight,
        first_moment.transpose(1, 0, 2),
        second_moment.transpose(1, 0, 2),
    )
    mine = lax.dynamic_slice_in_dim(bases, lax.axis_index("fs") * rows, rows, 1)
    f32 = jnp.float32

    def down(base, k):
        return jnp.dot(base[k], dirs[k], preferred_element_type=f32) * scales[k, 0]

    def across(base, k):
        return (
            lax.dot_general(dirs[k], base[k], (((0,), (1,)), ((), ())), preferred_element_type=f32)
            * scales[k, 0]
        )

    step_forget, step_value, step_out = down(mine, 0), down(mine, 1), across(mine, 2)
    return (
        forget_weight - 0.01 * step_forget,
        value_weight - 0.01 * step_value,
        out_weight - 0.01 * step_out,
        (old_f.astype(f32) - 0.01 * down(bases, 0)).astype(jnp.bfloat16),
        (old_v.astype(f32) - 0.01 * down(bases, 1)).astype(jnp.bfloat16),
        (old_o.astype(f32) - 0.01 * across(bases, 2)).astype(jnp.bfloat16),
        one.transpose(1, 0, 2),
        two.transpose(1, 0, 2),
        step_forget,
        step_value,
        step_out,
    )


def solution(mesh):
    placed = (
        P("fs", None),
        P("fs", "tp"),
        P("fs", "tp"),
        P("fs", "tp"),
        P("fs", None),
        P("fs", "tp"),
        P("fs", "tp"),
        P("tp", "fs"),
        P(),
        P("fs", None, "tp"),
        P("fs", None, "tp"),
    )
    return jax.shard_map(
        on_device,
        mesh=mesh,
        in_specs=placed,
        out_specs=(
            P("fs", "tp"),
            P("fs", "tp"),
            P("tp", "fs"),
            P(None, "tp"),
            P(None, "tp"),
            P("tp", None),
            P("fs", None, "tp"),
            P("fs", None, "tp"),
            P("fs", "tp"),
            P("fs", "tp"),
            P("tp", "fs"),
        ),
        check_vma=False,
    )
```

```python
import functools

import jax
import jax.numpy as jnp
from jax import lax
from jax.experimental import pallas as pl
from jax.experimental.pallas import tpu as pltpu
from jax.sharding import PartitionSpec as P

MESH = pl.DeviceIdType.MESH


def ring_index(place, size):
    back = lax.div(place, size // 2)
    return (1 - back) * 2 * place + back * (2 * (size - 1 - place) + 1)


def ring_place(index, size):
    odd = lax.rem(index, 2)
    half = lax.div(index, 2)
    return (1 - odd) * half + odd * (size - 1 - half)


def exchange_kernel(
    size,
    groups,
    factor,
    entries,
    x_hbm,
    oc_hbm,
    fc_hbm,
    vc_hbm,
    go_hbm,
    bases_hbm,
    fw_hbm,
    vw_hbm,
    ow_hbm,
    m1_hbm,
    m2_hbm,
    all_f,
    all_v,
    all_o,
    dirs_out,
    scale_ref,
    n1_ref,
    n2_ref,
    fw_ref,
    vw_ref,
    ow_ref,
    m1_ref,
    m2_ref,
    first_sem,
    x_buf,
    oc_buf,
    c_buf,
    b_buf,
    wf_buf,
    wv_buf,
    wo_buf,
    acc,
    part,
    got,
    mine,
    dirs,
    sums,
    load_sem,
    base_sem,
    put_sem,
    ring_send,
    ring_recv,
    part_send,
    part_recv,
    dir_send,
    dir_recv,
    sum_send,
    sum_recv,
):
    me = lax.axis_index("fs")
    mt = lax.axis_index("tp")
    place = ring_place(me, size)
    right = ring_index(lax.rem(place + 1, size), size)
    left = ring_index(lax.rem(place + size - 1, size), size)
    steps = size // 2
    tiles = load_sem.shape[1]
    tokens = x_buf.shape[0]
    rows_t = tokens // tiles
    rank_rows = m1_ref.shape[1]
    columns = m1_ref.shape[2]

    firsts = [
        pltpu.make_async_copy(src, dst, first_sem.at[i])
        for i, (src, dst) in enumerate(
            (
                (fw_hbm, fw_ref),
                (vw_hbm, vw_ref),
                (ow_hbm, ow_ref),
                (m1_hbm, m1_ref),
                (m2_hbm, m2_ref),
            )
        )
    ]
    for copy in firsts[:3]:
        copy.start()
    base_copies = [
        pltpu.make_async_copy(bases_hbm.at[k], b_buf.at[k], base_sem.at[k]) for k in range(3)
    ]

    def load(which, src, dst, tile):
        at = pl.ds(pl.multiple_of(tile * rows_t, rows_t), rows_t)
        return pltpu.make_async_copy(src.at[at, :], dst.at[at, :], load_sem.at[which, tile])

    streams = (
        (x_hbm, x_buf),
        (fc_hbm, c_buf.at[0]),
        (vc_hbm, c_buf.at[1]),
        (oc_hbm, oc_buf),
        (go_hbm, c_buf.at[2]),
    )
    base_copies[0].start()
    for tile in range(tiles):
        for which in (0, 1):
            load(which, *streams[which], tile).start()
    base_copies[1].start()
    for tile in range(tiles):
        load(2, *streams[2], tile).start()
    base_copies[2].start()
    for tile in range(tiles):
        for which in (3, 4):
            load(which, *streams[which], tile).start()

    for copy in firsts[3:]:
        copy.start()

    barrier = pltpu.get_barrier_semaphore()
    for j in range(1, size):
        pl.semaphore_signal(
            barrier, inc=1, device_id=(lax.rem(me + j, size), mt), device_id_type=MESH
        )
    for j in range(1, groups):
        pl.semaphore_signal(
            barrier, inc=1, device_id=(me, lax.rem(mt + j, groups)), device_id_type=MESH
        )
    for copy in firsts[:3]:
        copy.wait()
    wf_buf[...] = fw_ref[...].astype(jnp.bfloat16)
    wv_buf[...] = vw_ref[...].astype(jnp.bfloat16)
    wo_buf[...] = ow_ref[...].astype(jnp.bfloat16)
    pl.semaphore_wait(barrier, size - 1 + groups - 1)

    def row_block(ref, owner, half):
        rows = wf_buf.shape[0]
        start, count = owner * rows, rows
        if half is not None:
            count = rows // 2
            start = start + half * count
        return ref.at[pl.ds(pl.multiple_of(start, count), count), :]

    def column_block(ref, owner, half):
        width = wo_buf.shape[1]
        lanes = pl.ds(pl.multiple_of(owner * width, width), width)
        height = wo_buf.shape[0]
        if half is None:
            return ref.at[:, lanes]
        return ref.at[pl.ds(half * (height // 2), height // 2), lanes]

    def dir_block(k, owner, half):
        at = pl.ds(pl.multiple_of(owner * rank_rows, rank_rows), rank_rows)
        if half is None:
            return dirs.at[k, at, :]
        return dirs.at[k, at, pl.ds(half * (columns // 2), columns // 2)]

    items = (
        (wf_buf, functools.partial(row_block, all_f)),
        (wv_buf, functools.partial(row_block, all_v)),
        (wo_buf, functools.partial(column_block, all_o)),
    )

    def hop(view, own, send_sem, recv_sem, item, step, way):
        sign = 1 if way == 0 else size - 1
        owner = ring_index(lax.rem(place + (size - sign) * (step - 1), size), size)
        half = way if step == steps else None
        dst = view(owner, half)
        src = own if own is not None and step == 1 and half is None else dst
        return pltpu.make_async_remote_copy(
            src_ref=src,
            dst_ref=dst,
            send_sem=send_sem.at[way, item, step - 1],
            recv_sem=recv_sem.at[way, item, step - 1],
            device_id=(right if way == 0 else left, mt),
            device_id_type=MESH,
        )

    def weight_hop(item, step, way):
        own, view = items[item]
        return hop(view, own, ring_send, ring_recv, item, step, way)

    def dir_hop(k, step, way):
        own = mine.at[k]
        return hop(functools.partial(dir_block, k), own, dir_send, dir_recv, k, step, way)

    puts = []
    for item in range(3):
        own, view = items[item]
        put = pltpu.make_async_copy(own, view(me, None), put_sem.at[item])
        put.start()
        puts.append(put)
        for way in range(2):
            weight_hop(item, 1, way).start()

    forwards = [(step, item) for step in range(2, steps + 1) for item in range(3)]

    def pump(count):
        for _ in range(min(count, len(forwards))):
            step, item = forwards.pop(0)
            for way in range(2):
                weight_hop(item, step - 1, way).wait_recv()
                weight_hop(item, step, way).start()

    def part_copy(k, j):
        owner = lax.rem(me + j, size)
        at = pl.ds(pl.multiple_of(owner * rank_rows, rank_rows), rank_rows)
        return pltpu.make_async_remote_copy(
            src_ref=part.at[k, at, :],
            dst_ref=got.at[k, j - 1],
            send_sem=part_send.at[k, j - 1],
            recv_sem=part_recv.at[k, j - 1],
            device_id=(owner, mt),
            device_id_type=MESH,
        )

    own_rows = pl.ds(pl.multiple_of(me * rank_rows, rank_rows), rank_rows)

    def combine(k):
        projected = acc[k, own_rows, :] * factor
        for j in range(1, size):
            part_copy(k, j).wait_recv()
            projected = projected + got[k, j - 1].astype(jnp.float32)
        one = 0.9 * m1_ref[k] + 0.1 * projected
        two = 0.9 * m2_ref[k] + 0.1 * projected * projected
        n1_ref[k] = one
        n2_ref[k] = two
        rounded = (one / (jnp.sqrt(two) + 1e-08)).astype(jnp.bfloat16)
        mine[k] = rounded
        dirs[k, own_rows, :] = rounded
        for way in range(2):
            dir_hop(k, 1, way).start()

    for k in range(3):
        base_copies[k].wait()
        left_which, right_which = ((0, 1), (0, 2), (3, 4))[k]
        source = x_buf if k < 2 else oc_buf
        acc[k] = jnp.zeros(acc.shape[1:], acc.dtype)

        def tile_body(tile, carry, k=k, left_which=left_which, right_which=right_which, source=source):
            at = pl.ds(pl.multiple_of(tile * rows_t, rows_t), rows_t)
            if k != 1:
                load(left_which, *streams[left_which], tile).wait()
            reduced = jnp.dot(
                source[at, :], b_buf[k], preferred_element_type=jnp.float32
            ).astype(jnp.bfloat16)
            load(right_which, *streams[right_which], tile).wait()
            acc[k] += lax.dot_general(
                reduced,
                c_buf[k, at, :],
                (((0,), (0,)), ((), ())),
                preferred_element_type=jnp.float32,
            )
            return carry

        lax.fori_loop(0, tiles, tile_body, 0)
        part[k] = (acc[k] * factor).astype(jnp.bfloat16)
        for j in range(1, size):
            part_copy(k, j).start()
        pump(1)
        if k == 1:
            for copy in firsts[3:]:
                copy.wait()
        if k > 0:
            combine(k - 1)

    pump(1)
    combine(2)
    pump(2)
    for step in range(2, steps + 1):
        for k in range(3):
            for way in range(2):
                dir_hop(k, step - 1, way).wait_recv()
                dir_hop(k, step, way).start()
        if step == 3:
            pump(3)
    pump(len(forwards))
    for k in range(3):
        for way in range(2):
            dir_hop(k, steps, way).wait_recv()

    dirs_put = pltpu.make_async_copy(dirs, dirs_out, put_sem.at[3])
    dirs_put.start()

    row = lax.broadcasted_iota(jnp.int32, scale_ref.shape, 0)
    tile_sum = jnp.zeros(scale_ref.shape, jnp.float32)
    for k in range(3):
        values = dirs[k].astype(jnp.float32)
        tile_sum = tile_sum + jnp.where(row == k, jnp.sum(values * values), 0.0)
    sums[0] = tile_sum

    def sum_copy(j):
        return pltpu.make_async_remote_copy(
            src_ref=sums.at[0],
            dst_ref=sums.at[j],
            send_sem=sum_send.at[j],
            recv_sem=sum_recv.at[j],
            device_id=(me, lax.rem(mt + j, groups)),
            device_id_type=MESH,
        )

    for j in range(1, groups):
        sum_copy(j).start()
    total = tile_sum
    for j in range(1, groups):
        sum_copy(j).wait_recv()
        total = total + sums[j]
    scale_ref[...] = lax.rsqrt(total / entries + 1.0)

    for item in range(3):
        for way in range(2):
            weight_hop(item, steps, way).wait_recv()
    for put in puts:
        put.wait()
    dirs_put.wait()
    for k in range(3):
        for step in range(1, steps + 1):
            for way in range(2):
                weight_hop(k, step, way).wait_send()
                dir_hop(k, step, way).wait_send()
        for j in range(1, size):
            part_copy(k, j).wait_send()
    for j in range(1, groups):
        sum_copy(j).wait_send()


def exchange(size, groups, x, oc, fc, vc, go, bases, fw, vw, ow, m1, m2):
    tokens, width = x.shape
    rank = bases.shape[2]
    rows, columns = fw.shape
    rank_rows = m1.shape[1]
    steps = size // 2
    tiles = 4
    bf16, f32 = jnp.bfloat16, jnp.float32
    hbm = pl.BlockSpec(memory_space=pl.ANY)
    vmem = pl.BlockSpec(memory_space=pltpu.VMEM)
    dma = pltpu.SemaphoreType.DMA
    kernel = functools.partial(
        exchange_kernel,
        size,
        groups,
        float(tokens * size) ** (-0.5),
        float(rank * columns * groups),
    )
    return pl.pallas_call(
        kernel,
        out_shape=(
            jax.ShapeDtypeStruct((rows * size, columns), bf16),
            jax.ShapeDtypeStruct((rows * size, columns), bf16),
            jax.ShapeDtypeStruct((ow.shape[0], ow.shape[1] * size), bf16),
            jax.ShapeDtypeStruct((3, rank, columns), bf16),
            jax.ShapeDtypeStruct((8, 128), f32),
            jax.ShapeDtypeStruct(m1.shape, f32),
            jax.ShapeDtypeStruct(m2.shape, f32),
        ),
        in_specs=[pl.BlockSpec(memory_space=pltpu.HBM)] * 11,
        out_specs=(hbm,) * 4 + (vmem,) * 3,
        scratch_shapes=[
            pltpu.VMEM(fw.shape, f32),
            pltpu.VMEM(vw.shape, f32),
            pltpu.VMEM(ow.shape, f32),
            pltpu.VMEM(m1.shape, f32),
            pltpu.VMEM(m2.shape, f32),
            dma((5,)),
            pltpu.VMEM(x.shape, bf16),
            pltpu.VMEM(oc.shape, bf16),
            pltpu.VMEM((3, tokens, columns), bf16),
            pltpu.VMEM(bases.shape, bf16),
            pltpu.VMEM(fw.shape, bf16),
            pltpu.VMEM(vw.shape, bf16),
            pltpu.VMEM(ow.shape, bf16),
            pltpu.VMEM((3, rank, columns), f32),
            pltpu.VMEM((3, rank, columns), bf16),
            pltpu.VMEM((3, size - 1, rank_rows, columns), bf16),
            pltpu.VMEM((3, rank_rows, columns), bf16),
            pltpu.VMEM((3, rank, columns), bf16),
            pltpu.VMEM((groups, 8, 128), f32),
            dma((5, tiles)),
            dma((3,)),
            dma((4,)),
            dma((2, 3, steps)),
            dma((2, 3, steps)),
            dma((3, size - 1)),
            dma((3, size - 1)),
            dma((2, 3, steps)),
            dma((2, 3, steps)),
            dma((groups,)),
            dma((groups,)),
        ],
        compiler_params=pltpu.CompilerParams(
            collective_id=0, has_side_effects=True, vmem_limit_bytes=54 * 1024 * 1024
        ),
    )(x, oc, fc, vc, go, bases, fw, vw, ow, m1, m2)


def finish_kernel(
    scale_hbm,
    dirs_hbm,
    f_hbm,
    v_hbm,
    o_hbm,
    n1_hbm,
    n2_hbm,
    bases_hbm,
    fw_hbm,
    vw_hbm,
    ow_hbm,
    new_f,
    new_v,
    new_o,
    copy_f,
    copy_v,
    copy_o,
    n1_out,
    n2_out,
    step_f,
    step_v,
    step_o,
    scale_ref,
    dirs_ref,
    bases_ref,
    fw_ref,
    vw_ref,
    ow_ref,
    f_ref,
    v_ref,
    o_ref,
    n1_ref,
    n2_ref,
    small_sem,
    load_sem,
    cf_buf,
    cv_buf,
    co_buf,
    down_buf,
    across_buf,
    tile_sem,
    own_sem,
):
    tiles = tile_sem.shape[1]
    rows = f_ref.shape[0] // tiles
    smalls = [
        pltpu.make_async_copy(src, dst, small_sem.at[i])
        for i, (src, dst) in enumerate(
            (
                (dirs_hbm, dirs_ref),
                (scale_hbm, scale_ref),
                (bases_hbm, bases_ref),
                (fw_hbm, fw_ref),
                (vw_hbm, vw_ref),
                (ow_hbm, ow_ref),
                (n1_hbm, n1_ref),
                (n2_hbm, n2_ref),
            )
        )
    ]
    loads = []
    for tile in range(tiles):
        at = pl.ds(tile * rows, rows)
        views = (
            (f_hbm.at[at, :], f_ref.at[at, :]),
            (v_hbm.at[at, :], v_ref.at[at, :]),
            (o_hbm.at[:, at], o_ref.at[:, at]),
        )
        loads.append(
            [
                pltpu.make_async_copy(src, dst, load_sem.at[i, tile])
                for i, (src, dst) in enumerate(views)
            ]
        )
    for copy in smalls:
        copy.start()
    for group in loads:
        for copy in group:
            copy.start()
    for copy in smalls[:6]:
        copy.wait()
    copies = []

    def put(src, dst, sem):
        copy = pltpu.make_async_copy(src, dst, sem)
        copy.start()
        copies.append(copy)

    def down(rows, k):
        step = jnp.dot(bases_ref[k, rows, :], dirs_ref[k], preferred_element_type=jnp.float32)
        return step * scale_ref[k : k + 1, 0:1]

    def across(rows):
        step = lax.dot_general(
            dirs_ref[2],
            bases_ref[2, rows, :],
            (((0,), (1,)), ((), ())),
            preferred_element_type=jnp.float32,
        )
        return step * scale_ref[2:3, 0:1]

    own = fw_ref.shape[0]
    me = pl.ds(pl.multiple_of(lax.axis_index("fs") * own, own), own)
    for k, weight, new, out in ((0, fw_ref, new_f, step_f), (1, vw_ref, new_v, step_v)):
        step = down(me, k)
        down_buf[2 * k] = step
        put(down_buf.at[2 * k], out, own_sem.at[2 * k])
        down_buf[2 * k + 1] = weight[...] - 0.01 * step
        put(down_buf.at[2 * k + 1], new, own_sem.at[2 * k + 1])
    step = across(me)
    across_buf[0] = step
    put(across_buf.at[0], step_o, own_sem.at[4])
    across_buf[1] = ow_ref[...] - 0.01 * step
    put(across_buf.at[1], new_o, own_sem.at[5])

    for copy in smalls[6:]:
        copy.wait()
    put(n1_ref, n1_out, own_sem.at[6])
    put(n2_ref, n2_out, own_sem.at[7])

    for tile in range(tiles):
        at = pl.ds(tile * rows, rows)
        for copy in loads[tile]:
            copy.wait()
        for k, old, buf, out in ((0, f_ref, cf_buf, copy_f), (1, v_ref, cv_buf, copy_v)):
            value = old[at, :].astype(jnp.float32) - 0.01 * down(at, k)
            buf[at, :] = value.astype(jnp.bfloat16)
            put(buf.at[at, :], out.at[at, :], tile_sem.at[k, tile])
        value = o_ref[:, at].astype(jnp.float32) - 0.01 * across(at)
        co_buf[:, at] = value.astype(jnp.bfloat16)
        put(co_buf.at[:, at], copy_o.at[:, at], tile_sem.at[2, tile])
    for copy in copies:
        copy.wait()


def finish(scales, dirs, bases, old_f, old_v, old_o, fw, vw, ow, one, two):
    tiles = 4
    depth, columns = old_f.shape
    rank = bases.shape[2]
    dma = pltpu.SemaphoreType.DMA
    hbm = pl.BlockSpec(memory_space=pltpu.HBM)
    outs = (fw, vw, ow, old_f, old_v, old_o, one, two, fw, vw, ow)
    return pl.pallas_call(
        finish_kernel,
        out_shape=tuple(jax.ShapeDtypeStruct(a.shape, a.dtype) for a in outs),
        in_specs=[hbm] * 11,
        out_specs=(pl.BlockSpec(memory_space=pltpu.HBM),) * 11,
        scratch_shapes=[
            pltpu.VMEM(scales.shape, jnp.float32),
            pltpu.VMEM(dirs.shape, jnp.bfloat16),
            pltpu.VMEM(bases.shape, jnp.bfloat16),
            pltpu.VMEM(fw.shape, jnp.float32),
            pltpu.VMEM(vw.shape, jnp.float32),
            pltpu.VMEM(ow.shape, jnp.float32),
            pltpu.VMEM(old_f.shape, jnp.bfloat16),
            pltpu.VMEM(old_v.shape, jnp.bfloat16),
            pltpu.VMEM(old_o.shape, jnp.bfloat16),
            pltpu.VMEM(one.shape, jnp.float32),
            pltpu.VMEM(two.shape, jnp.float32),
            dma((8,)),
            dma((3, tiles)),
            pltpu.VMEM(old_f.shape, jnp.bfloat16),
            pltpu.VMEM(old_v.shape, jnp.bfloat16),
            pltpu.VMEM(old_o.shape, jnp.bfloat16),
            pltpu.VMEM((4,) + fw.shape, jnp.float32),
            pltpu.VMEM((2,) + ow.shape, jnp.float32),
            dma((3, tiles)),
            dma((8,)),
        ],
        compiler_params=pltpu.CompilerParams(vmem_limit_bytes=56 * 1024 * 1024),
        cost_estimate=pl.CostEstimate(
            flops=6 * depth * rank * columns, bytes_accessed=16 * depth * columns, transcendentals=0
        ),
    )(scales, dirs, old_f, old_v, old_o, one, two, bases, fw, vw, ow)


def on_device(
    normed_input,
    forget_cot,
    value_cot,
    gated_output,
    output_cot,
    forget_weight,
    value_weight,
    out_weight,
    bases,
    first_moment,
    second_moment,
):
    size, groups = lax.axis_size("fs"), lax.axis_size("tp")
    old_f, old_v, old_o, dirs, scales, one, two = exchange(
        size,
        groups,
        normed_input,
        output_cot,
        forget_cot,
        value_cot,
        gated_output,
        bases,
        forget_weight,
        value_weight,
        out_weight,
        first_moment.transpose(1, 0, 2),
        second_moment.transpose(1, 0, 2),
    )
    outs = finish(
        scales,
        dirs,
        bases,
        old_f,
        old_v,
        old_o,
        forget_weight,
        value_weight,
        out_weight,
        one,
        two,
    )
    return (
        *outs[:6],
        outs[6].transpose(1, 0, 2),
        outs[7].transpose(1, 0, 2),
        *outs[8:],
    )


def solution(mesh):
    placed = (
        P("fs", None),
        P("fs", "tp"),
        P("fs", "tp"),
        P("fs", "tp"),
        P("fs", None),
        P("fs", "tp"),
        P("fs", "tp"),
        P("tp", "fs"),
        P(),
        P("fs", None, "tp"),
        P("fs", None, "tp"),
    )
    return jax.shard_map(
        on_device,
        mesh=mesh,
        in_specs=placed,
        out_specs=(
            P("fs", "tp"),
            P("fs", "tp"),
            P("tp", "fs"),
            P(None, "tp"),
            P(None, "tp"),
            P("tp", None),
            P("fs", None, "tp"),
            P("fs", None, "tp"),
            P("fs", "tp"),
            P("fs", "tp"),
            P("tp", "fs"),
        ),
        check_vma=False,
    )
```
